32 devices in a mesh: grp: 2 (over y), fs: 4 (over z), tp: 4 (over x, core).
Axes of the slice: x: 2, y: 2, z: 4, core: 2. Of those that a mesh axis runs over, the one named last changes fastest.
Arguments:
- tokens: bfloat16 [8192, 2048], P(('grp', 'fs')), parts along dimension 0, may hold values from -6 to 6
- mixer_gain: float32 [2048], replicated, may hold values from 0.1 to 1.9
- outer_weight: float32 [2048, 2048], P('fs', 'tp'), may hold values from -0.125 to 0.125
- inner_weight: float32 [2048, 2048], P('fs', 'tp'), may hold values from -0.125 to 0.125
- value_weight: float32 [2048, 2048], P('fs', 'tp'), may hold values from -0.125 to 0.125
- filter_taps: float32 [3, 2048], P(None, 'tp'), may hold values from -3.5 to 3.5
- mixer_weight: float32 [2048, 2048], P('tp', 'fs'), may hold values from -0.125 to 0.125
- outer_scale: float32 [4, 512], P('tp', 'fs'), may hold values from 0.5 to 2
- inner_scale: float32 [4, 512], P('tp', 'fs'), may hold values from 0.5 to 2
- value_scale: float32 [4, 512], P('tp', 'fs'), may hold values from 0.5 to 2
- mixer_scale: float32 [1, 2048], P(None, 'fs'), may hold values from 0.5 to 2
Outputs:
- layer_out: bfloat16 [8192, 2048], P(('grp', 'fs', 'tp')), parts along dimension 0
The draws below stay inside these ranges and needn't reach their ends.
There are 2 independent parts, one for each index of `grp`. The reference program is written for one: setup_inputs(seed, part) draws one part's arguments, and reference() takes and returns one part's arrays. A program takes and returns all parts, laid end to end along the dimension named above; an argument that names none is the same for every part. Nothing has to cross between parts.
All inputs are finite; a program needn't handle non-finite values.
Results may differ from the reference program's by a relative error of at most 0.014.
Values may be sent and summed in bfloat16 or wider, within the bound.
A program may use at most 64 MiB of HBM per device.

```python
import math
import jax
import jax.numpy as jnp
from jax import lax

D = 2048
DC = 2048
SEQ_LEN = 1024
TOKENS = 4096
N_FS = 4
N_TP = 4


def levels(key, dims, shards, smallest, top_value):
    factor_of = 1.0
    for axis_at, blocks in shards:
        heights = jax.random.uniform(jax.random.fold_in(jax.random.fold_in(key, 6), axis_at), (blocks,), jnp.float32, smallest / len(shards), top_value / len(shards))
        factor_of = factor_of * jnp.repeat(jnp.exp(heights), dims[axis_at] // blocks).reshape((-1,) + (1,) * (len(dims) - 1 - axis_at))
    return factor_of


def centred(stream_key, dims, scale, reach, cuts=(), held_as=jnp.bfloat16):
    drawn = scale * jax.random.normal(stream_key, dims, jnp.float32)
    if cuts:
        drawn = drawn * levels(stream_key, dims, cuts, -0.22, 0.18)
    return jnp.clip(drawn, -reach, reach).astype(held_as)


def setup_inputs(seed: int = 0, part: int = 0) -> dict:
    streams_of = jax.random.split(jax.random.key(seed), 12)
    own_keys = jax.random.split(jax.random.fold_in(streams_of[11], part), 12)
    tokens = centred(own_keys[0], (TOKENS, D), 1.0, 6.0, ((0, 4),))
    mixer_gain = jnp.clip(1.0 + 0.18 * jax.random.normal(streams_of[1], (D,), jnp.float32), 0.1, 1.9)
    outer_weight = centred(streams_of[2], (D, DC), D ** -0.5, 0.125, ((0, 4), (1, 4)), jnp.float32)
    inner_weight = centred(streams_of[3], (D, DC), D ** -0.5, 0.125, ((0, 4), (1, 4)), jnp.float32)
    value_weight = centred(streams_of[4], (D, DC), D ** -0.5, 0.125, ((0, 4), (1, 4)), jnp.float32)
    filter_taps = centred(streams_of[5], (3, DC), 3 ** -0.5, 3.5, ((1, 4),), jnp.float32)
    mixer_weight = centred(streams_of[6], (DC, D), DC ** -0.5, 0.125, ((0, 4), (1, 4)), jnp.float32)
    outer_scale = jnp.clip(jnp.exp(math.log(2.0) - 1.3862944 * jax.random.uniform(streams_of[7], (N_TP, DC // N_TP), jnp.float32) ** levels(streams_of[7], (N_TP, DC // N_TP), ((0, 4), (1, 4)), -0.2, 0.2)), 0.5, 2.0)
    inner_scale = jnp.clip(jnp.exp(math.log(2.0) - 1.3862944 * jax.random.uniform(streams_of[8], (N_TP, DC // N_TP), jnp.float32) ** levels(streams_of[8], (N_TP, DC // N_TP), ((0, 4), (1, 4)), -0.2, 0.2)), 0.5, 2.0)
    value_scale = jnp.clip(jnp.exp(math.log(2.0) - 1.3862944 * jax.random.uniform(streams_of[9], (N_TP, DC // N_TP), jnp.float32) ** levels(streams_of[9], (N_TP, DC // N_TP), ((0, 4), (1, 4)), -0.2, 0.2)), 0.5, 2.0)
    mixer_scale = jnp.clip(jnp.exp(math.log(2.0) - 1.3862944 * jax.random.uniform(streams_of[10], (1, D), jnp.float32) ** levels(streams_of[10], (1, D), ((1, 4),), -0.2, 0.2)), 0.5, 2.0)
    return dict(tokens=tokens, mixer_gain=mixer_gain, outer_weight=outer_weight, inner_weight=inner_weight, value_weight=value_weight, filter_taps=filter_taps, mixer_weight=mixer_weight, outer_scale=outer_scale, inner_scale=inner_scale, value_scale=value_scale, mixer_scale=mixer_scale)


EPS = 1e-06

def normed(rows, gain):
    values = rows.astype(jnp.float32)
    inverse = lax.rsqrt(lax.optimization_barrier(jnp.mean(values * values, axis=-1, keepdims=True)) + EPS)
    return (values * inverse * gain).astype(jnp.bfloat16)

def project(left, weight, scale):
    return jnp.dot(left, weight.astype(jnp.bfloat16), preferred_element_type=jnp.float32) * scale.reshape(-1)

def rounded(values):
    return lax.optimization_barrier(values.astype(jnp.bfloat16)).astype(jnp.float32)

def summed_blocks(hidden, weight, scale):
    width = hidden.shape[1] // N_TP
    total = jnp.zeros((hidden.shape[0], weight.shape[1]), jnp.float32)
    for index in range(N_TP):
        part = project(hidden[:, index * width:(index + 1) * width], weight[index * width:(index + 1) * width], scale)
        total = total + rounded(part)
    return total

def reference(tokens, mixer_gain, outer_weight, inner_weight, value_weight, filter_taps, mixer_weight, outer_scale, inner_scale, value_scale, mixer_scale):
    normal_rows = normed(tokens, mixer_gain)
    outer = rounded(project(normal_rows, outer_weight, outer_scale))
    inner = rounded(project(normal_rows, inner_weight, inner_scale))
    value = rounded(project(normal_rows, value_weight, value_scale))
    product = (inner * value).reshape(N_FS, SEQ_LEN, DC)
    padded = jnp.pad(product, ((0, 0), (2, 0), (0, 0)))
    filtered = filter_taps[0] * padded[:, 0:SEQ_LEN] + filter_taps[1] * padded[:, 1:SEQ_LEN + 1] + filter_taps[2] * padded[:, 2:]
    gated = (outer * filtered.reshape(TOKENS, DC)).astype(jnp.bfloat16)
    return summed_blocks(gated, mixer_weight, mixer_scale).astype(jnp.bfloat16)
```

```python
import functools

import jax
import jax.numpy as jnp
from jax import lax
from jax.experimental import pallas as pl
from jax.experimental.pallas import tpu as pltpu
from jax.sharding import PartitionSpec as P

EPS = 1e-06


def normed(rows, gain):
    values = rows.astype(jnp.float32)
    inverse = lax.rsqrt(jnp.mean(values * values, axis=-1, keepdims=True) + EPS)
    return (values * inverse * gain).astype(jnp.bfloat16)


def rounded(values):
    return lax.optimization_barrier(values.astype(jnp.bfloat16)).astype(jnp.float32)


def add_rows(left, piece):
    return jnp.dot(left, piece, preferred_element_type=jnp.float32)


def per_device(
    tokens,
    mixer_gain,
    outer_weight,
    inner_weight,
    value_weight,
    filter_taps,
    mixer_weight,
    outer_scale,
    inner_scale,
    value_scale,
    mixer_scale,
):
    gathered = (
        lax.all_gather(outer_scale, "fs", axis=1, tiled=True),
        lax.all_gather(inner_scale, "fs", axis=1, tiled=True),
        lax.all_gather(value_scale, "fs", axis=1, tiled=True),
        lax.all_gather(mixer_scale, "fs", axis=1, tiled=True),
    )
    outer_col, inner_col, value_col, mixer_col = [piece.reshape(-1) for piece in gathered]
    seq_rows = tokens.shape[0]
    normal_rows = normed(tokens, mixer_gain)

    def fold_one(piece):
        return add_rows(normal_rows, piece)

    outer_sum = fold_one(
        lax.all_gather(outer_weight.astype(jnp.bfloat16), "fs", axis=0, tiled=True)
    )
    inner_sum = fold_one(
        lax.all_gather(inner_weight.astype(jnp.bfloat16), "fs", axis=0, tiled=True)
    )
    value_sum = fold_one(
        lax.all_gather(value_weight.astype(jnp.bfloat16), "fs", axis=0, tiled=True)
    )
    outer = rounded(outer_sum * outer_col)
    inner = rounded(inner_sum * inner_col)
    value = rounded(value_sum * value_col)
    padded = jnp.pad(inner * value, ((2, 0), (0, 0)))
    filtered = (
        filter_taps[0] * padded[0:seq_rows]
        + filter_taps[1] * padded[1 : seq_rows + 1]
        + filter_taps[2] * padded[2:]
    )
    gated = (outer * filtered).astype(jnp.bfloat16)
    mixer_full = lax.all_gather(mixer_weight.astype(jnp.bfloat16), "fs", axis=1, tiled=True)
    return lax.psum_scatter(
        (jnp.dot(gated, mixer_full, preferred_element_type=jnp.float32) * mixer_col).astype(
            jnp.bfloat16
        ),
        "tp",
        scatter_dimension=0,
        tiled=True,
    )


MESH = pl.DeviceIdType.MESH
MATRICES = 4


def mixer_kernel(
    n,
    tokens_hbm,
    gain_ref,
    w0_hbm,
    w1_hbm,
    w2_hbm,
    taps_ref,
    w3_hbm,
    s0_ref,
    s1_ref,
    s2_ref,
    s3_ref,
    out_ref,
    toks,
    rows,
    stage,
    held,
    scales,
    outer_buf,
    inner_buf,
    product,
    gated,
    own_part,
    core_out,
    core_in,
    chip_out,
    chip_in,
    load_sem,
    zl_sem,
    zr_sem,
    zin_sem,
    yout_sem,
    yin_sem,
    sout_sem,
    sin_sem,
    cout_sem,
    cin_sem,
    xout_sem,
    xin_sem,
):
    z = lax.axis_index("fs")
    y = lax.axis_index("grp")
    t = lax.axis_index("tp")
    ntp = 4
    block, width = stage.shape[1], stage.shape[2]
    half = block // 2
    seq = rows.shape[0]
    tile = seq // ntp
    partner = t + 1 - 2 * lax.rem(t, 2)
    across = lax.rem(t + 2, ntp)
    x, core = t // 2, lax.rem(t, 2)
    weights = (w0_hbm, w1_hbm, w2_hbm, w3_hbm)

    loads = [
        pltpu.make_async_copy(weights[m], stage.at[m], load_sem.at[m]) for m in range(MATRICES)
    ]
    token_load = pltpu.make_async_copy(tokens_hbm, toks, load_sem.at[MATRICES])
    for load in loads:
        load.start()
    token_load.start()

    barrier = pltpu.get_barrier_semaphore()
    for d in range(1, n):
        pl.semaphore_signal(
            barrier, inc=1, device_id={"fs": lax.rem(z + d, n)}, device_id_type=MESH
        )
    for d in range(1, ntp):
        pl.semaphore_signal(
            barrier, inc=1, device_id={"tp": lax.rem(t + d, ntp)}, device_id_type=MESH
        )
    pl.semaphore_signal(barrier, inc=1, device_id={"grp": 1 - y}, device_id_type=MESH)

    q = s0_ref.shape[1]
    scales[z, :, 0:q] = s0_ref[...]
    scales[z, :, q : 2 * q] = s1_ref[...]
    scales[z, :, 2 * q : 3 * q] = s2_ref[...]
    scales[z, :, 3 * q :] = s3_ref[...]

    def cast(m):
        loads[m].wait()
        held[m, pl.ds(pl.multiple_of(z * block, block), block), :] = stage[m].astype(jnp.bfloat16)

    def part_of(m, b):
        return held.at[m, pl.ds(pl.multiple_of(b * block + y * half, half), half), :]

    def other_of(m, b):
        return held.at[m, pl.ds(pl.multiple_of(b * block + (1 - y) * half, half), half), :]

    def to_left(m, b):
        return pltpu.make_async_remote_copy(
            src_ref=part_of(m, b),
            dst_ref=part_of(m, b),
            send_sem=zl_sem.at[m, b],
            recv_sem=zin_sem.at[m, b],
            device_id={"fs": z - 1},
            device_id_type=MESH,
        )

    def to_right(m, b):
        return pltpu.make_async_remote_copy(
            src_ref=part_of(m, b),
            dst_ref=part_of(m, b),
            send_sem=zr_sem.at[m, b],
            recv_sem=zin_sem.at[m, b],
            device_id={"fs": z + 1},
            device_id_type=MESH,
        )

    def to_twin(m, b):
        return pltpu.make_async_remote_copy(
            src_ref=part_of(m, b),
            dst_ref=part_of(m, b),
            send_sem=yout_sem.at[m, b],
            recv_sem=yin_sem.at[m, b],
            device_id={"grp": 1 - y},
            device_id_type=MESH,
        )

    def from_twin(m, b):
        return pltpu.make_async_remote_copy(
            src_ref=other_of(m, b),
            dst_ref=other_of(m, b),
            send_sem=yout_sem.at[m, b],
            recv_sem=yin_sem.at[m, b],
            device_id={"grp": 1 - y},
            device_id_type=MESH,
        )

    def scale_copy(d):
        return pltpu.make_async_remote_copy(
            src_ref=scales.at[z],
            dst_ref=scales.at[z],
            send_sem=sout_sem.at[d],
            recv_sem=sin_sem.at[z],
            device_id={"fs": lax.rem(z + d, n)},
            device_id_type=MESH,
        )

    def scale_arrival(d):
        source = lax.rem(z + d, n)
        return pltpu.make_async_remote_copy(
            src_ref=scales.at[source],
            dst_ref=scales.at[source],
            send_sem=sout_sem.at[d],
            recv_sem=sin_sem.at[source],
            device_id={"fs": source},
            device_id_type=MESH,
        )

    def send_own(m):
        @pl.when(z >= 1)
        def _():
            to_left(m, z).start()

        @pl.when(z <= n - 2)
        def _():
            to_right(m, z).start()

    def relay(m, s):
        from_right, from_left = z + 1 + s, z - 1 - s

        @pl.when(from_right <= n - 1)
        def _():
            to_left(m, from_right).wait_recv()

            @pl.when(z >= 1)
            def _():
                to_left(m, from_right).start()

            to_twin(m, from_right).start()

        @pl.when(from_left >= 0)
        def _():
            to_right(m, from_left).wait_recv()

            @pl.when(z <= n - 2)
            def _():
                to_right(m, from_left).start()

            to_twin(m, from_left).start()

    def twin_arrival(m, s):
        @pl.when(z + 1 + s <= n - 1)
        def _():
            from_twin(m, z + 1 + s).wait_recv()

        @pl.when(z - 1 - s >= 0)
        def _():
            from_twin(m, z - 1 - s).wait_recv()

    def column(k):
        return jnp.concatenate([scales[b, :, k * q : (k + 1) * q] for b in range(n)], axis=1)

    def project(m, first, count):
        return jnp.dot(
            rows[first : first + count, :], held[m], preferred_element_type=jnp.float32
        ) * column(m)

    def project_tiles(m, target, start, stop):
        for i in range(start, stop):
            first = i * tile
            target[first : first + tile, :] = project(m, first, tile).astype(jnp.bfloat16)

    cast(0)
    cast(1)
    pl.semaphore_wait(barrier, n - 1 + ntp - 1 + 1)
    send_own(0)
    for d in range(1, n):
        scale_copy(d).start()
    cast(2)
    cast(3)

    token_load.wait()
    strip = seq // 8

    @pl.loop(0, 8)
    def _(i):
        at = pl.ds(pl.multiple_of(i * strip, strip), strip)
        rows[at, :] = normed(toks[at, :], gain_ref[...])

    for d in range(1, n):
        scale_arrival(d).wait_recv()

    product[0:8, :] = jnp.zeros((8, width), jnp.float32)

    def gate_tile(i):
        first = i * tile
        value = project(2, first, tile).astype(jnp.bfloat16).astype(jnp.float32)
        product[8 + first : 8 + first + tile, :] = (
            inner_buf[first : first + tile, :].astype(jnp.float32) * value
        )
        filtered = (
            taps_ref[0:1, :] * product[6 + first : 6 + first + tile, :]
            + taps_ref[1:2, :] * product[7 + first : 7 + first + tile, :]
            + taps_ref[2:3, :] * product[8 + first : 8 + first + tile, :]
        )
        outer = outer_buf[first : first + tile, :].astype(jnp.float32)
        gated[first : first + tile, :] = (outer * filtered).astype(jnp.bfloat16)

    def core_copy(b):
        return pltpu.make_async_remote_copy(
            src_ref=core_out.at[b],
            dst_ref=core_in.at[b],
            send_sem=cout_sem.at[b],
            recv_sem=cin_sem.at[b],
            device_id={"tp": partner},
            device_id_type=MESH,
        )

    def chip_copy(b):
        return pltpu.make_async_remote_copy(
            src_ref=chip_out.at[b],
            dst_ref=chip_in.at[b],
            send_sem=xout_sem.at[b],
            recv_sem=xin_sem.at[b],
            device_id={"tp": across},
            device_id_type=MESH,
        )

    def mix_rows(b, index):
        at = pl.ds(pl.multiple_of(index * tile, tile), tile)
        weight = held[3, pl.ds(pl.multiple_of(b * block, block), block), :]
        return (
            jnp.dot(gated[at, :], weight, preferred_element_type=jnp.float32)
            * scales[b, :, 3 * q :]
        )

    def mix(b):
        for k in range(2):
            core_out[b, k] = mix_rows(b, 2 * k + 1 - core).astype(jnp.bfloat16)
        core_copy(b).start()
        for k in range(2):
            own_part[b, k] = mix_rows(b, 2 * k + core)
        core_copy(b).wait_recv()
        chip_out[b] = (own_part[b, 1 - x] + core_in[b, 1 - x].astype(jnp.float32)).astype(
            jnp.bfloat16
        )
        chip_copy(b).start()

    def mix_arrived(s):
        @pl.loop(0, 2)
        def _(side):
            b = z + (1 + s) * (1 - 2 * side)

            @pl.when((b >= 0) & (b <= n - 1))
            def _():
                from_twin(3, b).wait_recv()
                mix(b)

    steps = [(m, s) for m in range(MATRICES) for s in range(n - 1)]
    work = {}
    for m, target in ((0, outer_buf), (1, inner_buf)):
        at = (m + 1) * (n - 1)
        work[at + 1] = [functools.partial(project_tiles, m, target, 0, 2)]
        work[at + 2] = [functools.partial(project_tiles, m, target, 2, 4)]
    last = 3 * (n - 1)
    work[last + 1] = [functools.partial(gate_tile, i) for i in range(2)]
    work[last + 2] = [functools.partial(gate_tile, i) for i in range(2, 4)]
    for at, (m, s) in enumerate(steps):
        relay(m, s)
        if s == n - 2 and m < MATRICES - 1:
            send_own(m + 1)
        if at >= 1 and steps[at - 1][0] < 3:
            twin_arrival(*steps[at - 1])
        for task in work.get(at, ()):
            task()
    mix(z)
    for s in range(n - 1):
        mix_arrived(s)

    @pl.loop(0, n)
    def _(b):
        chip_copy(b).wait_recv()
        out_ref[b] = (
            own_part[b, x]
            + core_in[b, x].astype(jnp.float32)
            + chip_in[b].astype(jnp.float32)
        ).astype(jnp.bfloat16)
        core_copy(b).wait_send()
        chip_copy(b).wait_send()

    for d in range(1, n):
        scale_copy(d).wait_send()
    for m in range(MATRICES):

        @pl.loop(0, n)
        def _(b):
            @pl.when((b >= z) & (z >= 1))
            def _():
                to_left(m, b).wait_send()

            @pl.when((b <= z) & (z <= n - 2))
            def _():
                to_right(m, b).wait_send()

            @pl.when(b != z)
            def _():
                to_twin(m, b).wait_send()


def fused_device(
    n,
    tokens,
    mixer_gain,
    outer_weight,
    inner_weight,
    value_weight,
    filter_taps,
    mixer_weight,
    outer_scale,
    inner_scale,
    value_scale,
    mixer_scale,
):
    seq, depth = tokens.shape
    block, width = outer_weight.shape
    tile = seq // 4
    whole = pl.BlockSpec(memory_space=pltpu.VMEM)
    anywhere = pl.BlockSpec(memory_space=pl.ANY)
    bf16, f32 = jnp.bfloat16, jnp.float32
    dma = pltpu.SemaphoreType.DMA
    scale_width = 3 * outer_scale.shape[1] + mixer_scale.shape[1]
    blocks = pl.pallas_call(
        functools.partial(mixer_kernel, n),
        out_shape=jax.ShapeDtypeStruct((n, tile, width), bf16),
        in_specs=[
            anywhere,
            whole,
            anywhere,
            anywhere,
            anywhere,
            whole,
            anywhere,
            whole,
            whole,
            whole,
            whole,
        ],
        out_specs=whole,
        scratch_shapes=[
            pltpu.VMEM((seq, depth), bf16),
            pltpu.VMEM((seq, depth), bf16),
            pltpu.VMEM((MATRICES, block, width), f32),
            pltpu.VMEM((MATRICES, n * block, width), bf16),
            pltpu.VMEM((n, 1, scale_width), f32),
            pltpu.VMEM((seq, width), bf16),
            pltpu.VMEM((seq, width), bf16),
            pltpu.VMEM((seq + 8, width), f32),
            pltpu.VMEM((seq, width), bf16),
            pltpu.VMEM((n, 2, tile, width), f32),
            pltpu.VMEM((n, 2, tile, width), bf16),
            pltpu.VMEM((n, 2, tile, width), bf16),
            pltpu.VMEM((n, tile, width), bf16),
            pltpu.VMEM((n, tile, width), bf16),
            dma((MATRICES + 1,)),
            dma((MATRICES, n)),
            dma((MATRICES, n)),
            dma((MATRICES, n)),
            dma((MATRICES, n)),
            dma((MATRICES, n)),
            dma((n,)),
            dma((n,)),
            dma((n,)),
            dma((n,)),
            dma((n,)),
            dma((n,)),
        ],
        compiler_params=pltpu.CompilerParams(
            collective_id=0, has_side_effects=True, vmem_limit_bytes=56 * 2**20
        ),
    )(
        tokens,
        mixer_gain.reshape(1, -1),
        outer_weight,
        inner_weight,
        value_weight,
        filter_taps,
        mixer_weight,
        outer_scale,
        inner_scale,
        value_scale,
        mixer_scale,
    )
    return blocks.transpose(1, 0, 2).reshape(tile, n * width)


def choose(mesh):
    n, ntp, groups = mesh.shape["fs"], mesh.shape["tp"], mesh.shape["grp"]

    def run(*args):
        tokens, weight, mixer, scale = args[0], args[2], args[6], args[7]
        fits = (
            groups == 2
            and ntp == 4
            and n == 4
            and weight.shape == mixer.shape
            and weight.shape[0] % 64 == 0
            and weight.shape[1] % 128 == 0
            and scale.shape[1] % 128 == 0
            and tokens.shape[0] % 256 == 0
        )
        return fused_device(n, *args) if fits else per_device(*args)

    return run


def solution(mesh):
    in_specs = (
        P(("grp", "fs"), None),
        P(),
        P("fs", "tp"),
        P("fs", "tp"),
        P("fs", "tp"),
        P(None, "tp"),
        P("tp", "fs"),
        P("tp", "fs"),
        P("tp", "fs"),
        P("tp", "fs"),
        P(None, "fs"),
    )
    out_specs = P(("grp", "fs", "tp"), None)
    return jax.shard_map(
        choose(mesh), mesh=mesh, in_specs=in_specs, out_specs=out_specs, check_vma=False
    )
```

```python
import functools

import jax
import jax.numpy as jnp
from jax import lax
from jax.experimental import pallas as pl
from jax.experimental.pallas import tpu as pltpu
from jax.sharding import PartitionSpec as P

EPS = 1e-06


def normed(rows, gain):
    values = rows.astype(jnp.float32)
    inverse = lax.rsqrt(jnp.mean(values * values, axis=-1, keepdims=True) + EPS)
    return (values * inverse * gain).astype(jnp.bfloat16)


def rounded(values):
    return lax.optimization_barrier(values.astype(jnp.bfloat16)).astype(jnp.float32)


def add_rows(left, piece):
    return jnp.dot(left, piece, preferred_element_type=jnp.float32)


def per_device(
    tokens,
    mixer_gain,
    outer_weight,
    inner_weight,
    value_weight,
    filter_taps,
    mixer_weight,
    outer_scale,
    inner_scale,
    value_scale,
    mixer_scale,
):
    gathered = (
        lax.all_gather(outer_scale, "fs", axis=1, tiled=True),
        lax.all_gather(inner_scale, "fs", axis=1, tiled=True),
        lax.all_gather(value_scale, "fs", axis=1, tiled=True),
        lax.all_gather(mixer_scale, "fs", axis=1, tiled=True),
    )
    outer_col, inner_col, value_col, mixer_col = [piece.reshape(-1) for piece in gathered]
    seq_rows = tokens.shape[0]
    normal_rows = normed(tokens, mixer_gain)

    def fold_one(piece):
        return add_rows(normal_rows, piece)

    outer_sum = fold_one(
        lax.all_gather(outer_weight.astype(jnp.bfloat16), "fs", axis=0, tiled=True)
    )
    inner_sum = fold_one(
        lax.all_gather(inner_weight.astype(jnp.bfloat16), "fs", axis=0, tiled=True)
    )
    value_sum = fold_one(
        lax.all_gather(value_weight.astype(jnp.bfloat16), "fs", axis=0, tiled=True)
    )
    outer = rounded(outer_sum * outer_col)
    inner = rounded(inner_sum * inner_col)
    value = rounded(value_sum * value_col)
    padded = jnp.pad(inner * value, ((2, 0), (0, 0)))
    filtered = (
        filter_taps[0] * padded[0:seq_rows]
        + filter_taps[1] * padded[1 : seq_rows + 1]
        + filter_taps[2] * padded[2:]
    )
    gated = (outer * filtered).astype(jnp.bfloat16)
    mixer_full = lax.all_gather(mixer_weight.astype(jnp.bfloat16), "fs", axis=1, tiled=True)
    return lax.psum_scatter(
        (jnp.dot(gated, mixer_full, preferred_element_type=jnp.float32) * mixer_col).astype(
            jnp.bfloat16
        ),
        "tp",
        scatter_dimension=0,
        tiled=True,
    )


MESH = pl.DeviceIdType.MESH
MATRICES = 4
SPLIT = 1
PIECES = MATRICES * SPLIT


def mixer_kernel(
    n,
    tokens_hbm,
    gain_ref,
    w0_hbm,
    w1_hbm,
    w2_hbm,
    taps_ref,
    w3_hbm,
    s0_ref,
    s1_ref,
    s2_ref,
    s3_ref,
    out_ref,
    toks,
    rows,
    stage,
    held,
    scales,
    outer_buf,
    inner_buf,
    product,
    gated,
    own_part,
    core_out,
    core_in,
    chip_out,
    chip_in,
    load_sem,
    zl_sem,
    zr_sem,
    zin_sem,
    yout_sem,
    yin_sem,
    sout_sem,
    sin_sem,
    cout_sem,
    cin_sem,
    xout_sem,
    xin_sem,
):
    z = lax.axis_index("fs")
    y = lax.axis_index("grp")
    t = lax.axis_index("tp")
    ntp = 4
    block, width = stage.shape[1], stage.shape[2]
    half = block // 2
    seq = rows.shape[0]
    tile = seq // ntp
    partner = t + 1 - 2 * lax.rem(t, 2)
    across = lax.rem(t + 2, ntp)
    x, core = t // 2, lax.rem(t, 2)
    weights = (w0_hbm, w1_hbm, w2_hbm, w3_hbm)

    loads = [
        pltpu.make_async_copy(weights[m], stage.at[m], load_sem.at[m]) for m in range(MATRICES)
    ]
    token_load = pltpu.make_async_copy(tokens_hbm, toks, load_sem.at[MATRICES])
    for load in loads:
        load.start()
    token_load.start()

    barrier = pltpu.get_barrier_semaphore()
    for d in range(1, n):
        pl.semaphore_signal(
            barrier, inc=1, device_id={"fs": lax.rem(z + d, n)}, device_id_type=MESH
        )
    for d in range(1, ntp):
        pl.semaphore_signal(
            barrier, inc=1, device_id={"tp": lax.rem(t + d, ntp)}, device_id_type=MESH
        )
    pl.semaphore_signal(barrier, inc=1, device_id={"grp": 1 - y}, device_id_type=MESH)

    q = s0_ref.shape[1]
    scales[z, :, 0:q] = s0_ref[...]
    scales[z, :, q : 2 * q] = s1_ref[...]
    scales[z, :, 2 * q : 3 * q] = s2_ref[...]
    scales[z, :, 3 * q :] = s3_ref[...]

    def cast(m):
        loads[m].wait()
        held[m, pl.ds(pl.multiple_of(z * block, block), block), :] = stage[m].astype(jnp.bfloat16)

    chunk = half // SPLIT

    def rows_of(p, b, side):
        first = b * block + side * half + (p % SPLIT) * chunk
        return held.at[p // SPLIT, pl.ds(pl.multiple_of(first, chunk), chunk), :]

    def part_of(p, b):
        return rows_of(p, b, y)

    def other_of(p, b):
        return rows_of(p, b, 1 - y)

    def to_left(m, b):
        return pltpu.make_async_remote_copy(
            src_ref=part_of(m, b),
            dst_ref=part_of(m, b),
            send_sem=zl_sem.at[m, b],
            recv_sem=zin_sem.at[m, b],
            device_id={"fs": z - 1},
            device_id_type=MESH,
        )

    def to_right(m, b):
        return pltpu.make_async_remote_copy(
            src_ref=part_of(m, b),
            dst_ref=part_of(m, b),
            send_sem=zr_sem.at[m, b],
            recv_sem=zin_sem.at[m, b],
            device_id={"fs": z + 1},
            device_id_type=MESH,
        )

    def to_twin(m, b):
        return pltpu.make_async_remote_copy(
            src_ref=part_of(m, b),
            dst_ref=part_of(m, b),
            send_sem=yout_sem.at[m, b],
            recv_sem=yin_sem.at[m, b],
            device_id={"grp": 1 - y},
            device_id_type=MESH,
        )

    def from_twin(m, b):
        return pltpu.make_async_remote_copy(
            src_ref=other_of(m, b),
            dst_ref=other_of(m, b),
            send_sem=yout_sem.at[m, b],
            recv_sem=yin_sem.at[m, b],
            device_id={"grp": 1 - y},
            device_id_type=MESH,
        )

    def scale_copy(d):
        return pltpu.make_async_remote_copy(
            src_ref=scales.at[z],
            dst_ref=scales.at[z],
            send_sem=sout_sem.at[d],
            recv_sem=sin_sem.at[z],
            device_id={"fs": lax.rem(z + d, n)},
            device_id_type=MESH,
        )

    def scale_arrival(d):
        source = lax.rem(z + d, n)
        return pltpu.make_async_remote_copy(
            src_ref=scales.at[source],
            dst_ref=scales.at[source],
            send_sem=sout_sem.at[d],
            recv_sem=sin_sem.at[source],
            device_id={"fs": source},
            device_id_type=MESH,
        )

    def send_own(m):
        @pl.when(z >= 1)
        def _():
            to_left(m, z).start()

        @pl.when(z <= n - 2)
        def _():
            to_right(m, z).start()

    def relay(m, s):
        from_right, from_left = z + 1 + s, z - 1 - s

        @pl.when(from_right <= n - 1)
        def _():
            to_left(m, from_right).wait_recv()

            @pl.when(z >= 1)
            def _():
                to_left(m, from_right).start()

            to_twin(m, from_right).start()

        @pl.when(from_left >= 0)
        def _():
            to_right(m, from_left).wait_recv()

            @pl.when(z <= n - 2)
            def _():
                to_right(m, from_left).start()

            to_twin(m, from_left).start()

    def twin_arrival(m, s):
        @pl.when(z + 1 + s <= n - 1)
        def _():
            from_twin(m, z + 1 + s).wait_recv()

        @pl.when(z - 1 - s >= 0)
        def _():
            from_twin(m, z - 1 - s).wait_recv()

    def column(k):
        return jnp.concatenate([scales[b, :, k * q : (k + 1) * q] for b in range(n)], axis=1)

    def project(m, first, count):
        return jnp.dot(
            rows[first : first + count, :], held[m], preferred_element_type=jnp.float32
        ) * column(m)

    def project_tiles(m, target, start, stop):
        for i in range(start, stop):
            first = i * tile
            target[first : first + tile, :] = project(m, first, tile).astype(jnp.bfloat16)

    cast(0)
    cast(1)
    pl.semaphore_wait(barrier, n - 1 + ntp - 1 + 1)
    for d in range(1, n):
        scale_copy(d).start()
    send_own(0)
    cast(2)
    cast(3)
    at_end = (z == 0) | (z == n - 1)

    @pl.when(at_end)
    def _():
        for p in range(1, PIECES):
            send_own(p)

    def send_own_inside(m):
        @pl.when(jnp.logical_not(at_end))
        def _():
            send_own(m)

    token_load.wait()
    strip = seq // 8

    @pl.loop(0, 8)
    def _(i):
        at = pl.ds(pl.multiple_of(i * strip, strip), strip)
        rows[at, :] = normed(toks[at, :], gain_ref[...])

    product[0:8, :] = jnp.zeros((8, width), jnp.float32)

    def gate_tile(i):
        first = i * tile
        value = project(2, first, tile).astype(jnp.bfloat16).astype(jnp.float32)
        product[8 + first : 8 + first + tile, :] = (
            inner_buf[first : first + tile, :].astype(jnp.float32) * value
        )
        filtered = (
            taps_ref[0:1, :] * product[6 + first : 6 + first + tile, :]
            + taps_ref[1:2, :] * product[7 + first : 7 + first + tile, :]
            + taps_ref[2:3, :] * product[8 + first : 8 + first + tile, :]
        )
        outer = outer_buf[first : first + tile, :].astype(jnp.float32)
        gated[first : first + tile, :] = (outer * filtered).astype(jnp.bfloat16)

    def core_copy(b):
        return pltpu.make_async_remote_copy(
            src_ref=core_out.at[b],
            dst_ref=core_in.at[b],
            send_sem=cout_sem.at[b],
            recv_sem=cin_sem.at[b],
            device_id={"tp": partner},
            device_id_type=MESH,
        )

    def chip_copy(b):
        return pltpu.make_async_remote_copy(
            src_ref=chip_out.at[b],
            dst_ref=chip_in.at[b],
            send_sem=xout_sem.at[b],
            recv_sem=xin_sem.at[b],
            device_id={"tp": across},
            device_id_type=MESH,
        )

    def mix_rows(b, index):
        at = pl.ds(pl.multiple_of(index * tile, tile), tile)
        weight = held[3, pl.ds(pl.multiple_of(b * block, block), block), :]
        return (
            jnp.dot(gated[at, :], weight, preferred_element_type=jnp.float32)
            * scales[b, :, 3 * q :]
        )

    def mix(b):
        for k in range(2):
            core_out[b, k] = mix_rows(b, 2 * k + 1 - core).astype(jnp.bfloat16)
        core_copy(b).start()
        for k in range(2):
            own_part[b, k] = mix_rows(b, 2 * k + core)
        core_copy(b).wait_recv()
        chip_out[b] = (own_part[b, 1 - x] + core_in[b, 1 - x].astype(jnp.float32)).astype(
            jnp.bfloat16
        )
        chip_copy(b).start()

    def mix_arrived(s):
        @pl.loop(0, 2)
        def _(side):
            b = z + (1 + s) * (1 - 2 * side)

            @pl.when((b >= 0) & (b <= n - 1))
            def _():
                for p in range(3 * SPLIT, PIECES):
                    from_twin(p, b).wait_recv()
                mix(b)

    def all_twins(m):
        for p in range(m * SPLIT, (m + 1) * SPLIT):
            for s in range(n - 1):
                twin_arrival(p, s)

    def outer_tiles(start, stop):
        project_tiles(0, outer_buf, start, stop)

    def inner_tiles(start, stop):
        project_tiles(1, inner_buf, start, stop)

    def scales_in():
        for d in range(1, n):
            scale_arrival(d).wait_recv()

    steps = [(p, s) for p in range(PIECES) for s in range(n - 1)]
    per_matrix = SPLIT * (n - 1)
    work = {
        per_matrix + SPLIT: [
            scales_in,
            functools.partial(all_twins, 0),
            functools.partial(outer_tiles, 0, 2),
        ],
        per_matrix + 2 * SPLIT: [functools.partial(outer_tiles, 2, 4)],
        2 * per_matrix + SPLIT: [
            functools.partial(all_twins, 1),
            functools.partial(inner_tiles, 0, 2),
        ],
        2 * per_matrix + 2 * SPLIT: [functools.partial(inner_tiles, 2, 4)],
        3 * per_matrix: [functools.partial(all_twins, 2)]
        + [functools.partial(gate_tile, i) for i in range(4)]
        + [functools.partial(mix, z)],
    }
    for at, (p, s) in enumerate(steps):
        relay(p, s)
        if s == n - 3 and p < PIECES - 1:
            send_own_inside(p + 1)
        for task in work.get(at, ()):
            task()
        if p == PIECES - 1 and s >= 1:
            mix_arrived(s - 1)
    mix_arrived(n - 2)

    @pl.loop(0, n)
    def _(b):
        chip_copy(b).wait_recv()
        out_ref[:, pl.ds(pl.multiple_of(b * width, width), width)] = (
            own_part[b, x]
            + core_in[b, x].astype(jnp.float32)
            + chip_in[b].astype(jnp.float32)
        ).astype(jnp.bfloat16)
        core_copy(b).wait_send()
        chip_copy(b).wait_send()

    for d in range(1, n):
        scale_copy(d).wait_send()
    for p in range(PIECES):

        @pl.loop(0, n)
        def _(b):
            @pl.when((b >= z) & (z >= 1))
            def _():
                to_left(p, b).wait_send()

            @pl.when((b <= z) & (z <= n - 2))
            def _():
                to_right(p, b).wait_send()

            @pl.when(b != z)
            def _():
                to_twin(p, b).wait_send()


def fused_device(
    n,
    tokens,
    mixer_gain,
    outer_weight,
    inner_weight,
    value_weight,
    filter_taps,
    mixer_weight,
    outer_scale,
    inner_scale,
    value_scale,
    mixer_scale,
):
    seq, depth = tokens.shape
    block, width = outer_weight.shape
    tile = seq // 4
    whole = pl.BlockSpec(memory_space=pltpu.VMEM)
    anywhere = pl.BlockSpec(memory_space=pl.ANY)
    bf16, f32 = jnp.bfloat16, jnp.float32
    dma = pltpu.SemaphoreType.DMA
    scale_width = 3 * outer_scale.shape[1] + mixer_scale.shape[1]
    return pl.pallas_call(
        functools.partial(mixer_kernel, n),
        out_shape=jax.ShapeDtypeStruct((tile, n * width), bf16),
        in_specs=[
            anywhere,
            whole,
            anywhere,
            anywhere,
            anywhere,
            whole,
            anywhere,
            whole,
            whole,
            whole,
            whole,
        ],
        out_specs=whole,
        scratch_shapes=[
            pltpu.VMEM((seq, depth), bf16),
            pltpu.VMEM((seq, depth), bf16),
            pltpu.VMEM((MATRICES, block, width), f32),
            pltpu.VMEM((MATRICES, n * block, width), bf16),
            pltpu.VMEM((n, 1, scale_width), f32),
            pltpu.VMEM((seq, width), bf16),
            pltpu.VMEM((seq, width), bf16),
            pltpu.VMEM((seq + 8, width), f32),
            pltpu.VMEM((seq, width), bf16),
            pltpu.VMEM((n, 2, tile, width), f32),
            pltpu.VMEM((n, 2, tile, width), bf16),
            pltpu.VMEM((n, 2, tile, width), bf16),
            pltpu.VMEM((n, tile, width), bf16),
            pltpu.VMEM((n, tile, width), bf16),
            dma((MATRICES + 1,)),
            dma((PIECES, n)),
            dma((PIECES, n)),
            dma((PIECES, n)),
            dma((PIECES, n)),
            dma((PIECES, n)),
            dma((n,)),
            dma((n,)),
            dma((n,)),
            dma((n,)),
            dma((n,)),
            dma((n,)),
        ],
        compiler_params=pltpu.CompilerParams(
            collective_id=0, has_side_effects=True, vmem_limit_bytes=56 * 2**20
        ),
    )(
        tokens,
        mixer_gain.reshape(1, -1),
        outer_weight,
        inner_weight,
        value_weight,
        filter_taps,
        mixer_weight,
        outer_scale,
        inner_scale,
        value_scale,
        mixer_scale,
    )


def choose(mesh):
    n, ntp, groups = mesh.shape["fs"], mesh.shape["tp"], mesh.shape["grp"]

    def run(*args):
        tokens, weight, mixer, scale = args[0], args[2], args[6], args[7]
        fits = (
            groups == 2
            and ntp == 4
            and n == 4
            and weight.shape == mixer.shape
            and weight.shape[0] % (32 * SPLIT) == 0
            and weight.shape[1] % 128 == 0
            and scale.shape[1] % 128 == 0
            and tokens.shape[0] % 256 == 0
        )
        return fused_device(n, *args) if fits else per_device(*args)

    return run


def solution(mesh):
    in_specs = (
        P(("grp", "fs"), None),
        P(),
        P("fs", "tp"),
        P("fs", "tp"),
        P("fs", "tp"),
        P(None, "tp"),
        P("tp", "fs"),
        P("tp", "fs"),
        P("tp", "fs"),
        P("tp", "fs"),
        P(None, "fs"),
    )
    out_specs = P(("grp", "fs", "tp"), None)
    return jax.shard_map(
        choose(mesh), mesh=mesh, in_specs=in_specs, out_specs=out_specs, check_vma=False
    )
```
